32 devices in a mesh: ep: 8 (over z, y), tp: 4 (over x, core).
Axes of the slice: x: 2, y: 2, z: 4, core: 2. Of those that a mesh axis runs over, the one named last changes fastest.
Arguments:
- tokens_first: bfloat16 [4096, 2048], P('ep'), may hold values from -6 to 6
- norm_gain_first: float32 [2048], replicated, may hold values from 0.1 to 1.9
- w_query: bfloat16 [2048, 512], P(None, 'tp'), may hold values from -0.125 to 0.125
- w_key: bfloat16 [2048, 512], P(None, 'tp'), may hold values from -0.125 to 0.125
- w_value: bfloat16 [2048, 1024], P(None, 'tp'), may hold values from -0.125 to 0.125
- w_outgate: bfloat16 [2048, 1024], P(None, 'tp'), may hold values from -0.125 to 0.125
- w_decay: bfloat16 [2048, 512], P(None, 'tp'), may hold values from -1 to 1
- decay_bias: float32 [64, 512], P('ep', 'tp'), may hold values from -1.3 to 12.5
- head_gain: float32 [1024], P('tp'), may hold values from 0.1 to 1.9
- w_mix_out: bfloat16 [1024, 2048], P('tp'), may hold values from -0.1875 to 0.1875
- tokens_second: bfloat16 [2048, 2048], P('ep'), may hold values from -6 to 6
- norm_gain_second: float32 [2048], replicated, may hold values from 0.1 to 1.9
- routes: int32 [2048, 2], P('ep'), may hold values from 0 to 7, all different within a row; in each aligned block of 256 rows (0 to 255, 256 to 511, ...) at most 128 rows name the same one
- route_logits: float32 [2048, 2], P('ep'), may hold values from -8 to 8
- expert_gate: bfloat16 [8, 2048, 3072], P('ep', None, 'tp'), may hold values from -0.125 to 0.125
- expert_up: bfloat16 [8, 2048, 3072], P('ep', None, 'tp'), may hold values from -0.125 to 0.125
- expert_down: bfloat16 [8, 3072, 2048], P('ep', 'tp'), may hold values from -0.109375 to 0.109375
Outputs:
- mixed_first: bfloat16 [4096, 2048], P(('ep', 'tp'))
- mixed_second: bfloat16 [2048, 2048], P('ep', 'tp')
The draws below stay inside these ranges and needn't reach their ends.
Inputs may be any that keep to these rules, and one draw needn't show every extreme that they name: In the rows of one index of ep (aligned blocks of 256 rows) no expert is named by more than 128 rows, a bound that some block reaches; the two routes of a row name different experts.
All inputs are finite; a program needn't handle non-finite values.
Results may differ from the reference program's by a relative error of at most 0.01.
Values may be sent and summed in bfloat16 or wider, within the bound.
A program may use at most 128 MiB of HBM per device.

```python
import math
import jax
import jax.numpy as jnp
import numpy as np
from jax import lax

D = 2048
HEADS = 8
KEY_DIM = 64
VALUE_DIM = 128
FFE = 3072
TOPK = 2
BLOCK = 64
ROWS_B = 256
QK_WIDTH = 512
V_WIDTH = 1024
EXPERTS = 8
TOKENS_A = 4096
TOKENS_B = 2048
NBLK = 64
CAP = 128
N_EP = 8
N_TP = 4


def draw_w_decay(key, part):
    limit = jnp.minimum(15.0 / jnp.sqrt(jnp.float32(D)), jnp.float32(1.0))
    entries = jax.random.normal(jax.random.fold_in(key, 11), (D, QK_WIDTH), jnp.float32) * (2.5 / jnp.sqrt(jnp.float32(D)))
    entries = jnp.clip(entries, -limit, limit)
    return entries.astype(jnp.bfloat16)


def draw_decay_bias(key, part):
    pick_key, slow_key, fast_key, block_key = jax.random.split(key, 4)
    slow_share = 0.5
    chosen = jax.random.uniform(pick_key, (QK_WIDTH,), jnp.float32) < slow_share
    slow_center = jnp.log(jnp.float32(0.86) * TOKENS_A)
    slow_base = slow_center + jax.random.uniform(slow_key, (QK_WIDTH,), jnp.float32, -0.5, 0.5)
    fast_base = jax.random.uniform(fast_key, (QK_WIDTH,), jnp.float32, -0.5, 1.5)
    channel_base = jnp.where(chosen, slow_base, fast_base)
    offset = jax.random.uniform(block_key, (NBLK, 1), jnp.float32, -0.8, 0.8)
    return (channel_base[None, :] + offset).astype(jnp.float32)


def block_scale(key, dims, pieces, smallest, high):
    level, own = 1.0, jax.random.fold_in(key, 6)
    for position, blocks in pieces:
        steps = jnp.exp(jax.random.uniform(jax.random.fold_in(own, position), (blocks,), jnp.float32, smallest / len(pieces), high / len(pieces)))
        level = level * jnp.repeat(steps, dims[position] // blocks).reshape([-1 if axis == position else 1 for axis in range(len(dims))])
    return level


def shared_out(own_key, own, number, rows, amount, top, bound, skew):
    order = jax.random.permutation(own_key, amount)
    crowded, common = portions_of(amount, rows * top, bound, skew, True), portions_of(amount, rows * top, bound, skew, False)
    places = jnp.arange(amount)

    def named(tallies, turn):
        used = int((tallies > 0).sum())
        fixed = max(1, used // 4)
        passed = fixed + (places - fixed + turn * (used - fixed)) % max(1, amount - fixed)
        return jnp.zeros((amount,), jnp.int32).at[order[jnp.where(places < fixed, places, passed)]].set(jnp.asarray(tallies, jnp.int32))

    tallies = jnp.where(number % 4 == 0, named(crowded, number // 4), named(common, number - number // 4 - 1))
    mixed = jax.random.permutation(jax.random.fold_in(own, 3), amount)
    source_of, taker = mixed[0:amount // 2 * 2:2], mixed[1:amount // 2 * 2:2]
    margin = jnp.minimum(tallies[source_of] - 1, bound - tallies[taker]) // 2
    margin = jnp.where((source_of == order[0]) | (taker == order[0]) | (tallies[taker] == 0), 0, jnp.maximum(margin, 0))
    passed = jax.random.randint(jax.random.fold_in(own, 4), (amount // 2,), 0, 1 << 20) % (margin + 1)
    tallies = tallies.at[source_of].add(-passed).at[taker].add(passed)
    labels = jnp.searchsorted(jnp.cumsum(tallies), jnp.arange(rows * top), side="right").astype(jnp.int32)
    grid = labels.reshape(top, rows).T
    grid = grid[jax.random.permutation(jax.random.fold_in(own, 1), rows)]
    turn = jax.random.randint(jax.random.fold_in(own, 2), (rows, 1), 0, top)
    return jnp.take_along_axis(grid, (jnp.arange(top)[None, :] + turn) % top, axis=1)


def portions_of(amount, total, reach, lean, full):
    loads = [(1 << 20) // math.isqrt(grade ** lean) + 1 for grade in range(1, amount + 1)]
    largest = reach if full else min(reach, max(-(-total // amount), total * loads[0] // sum(loads)))
    least = 1 if total - largest >= amount - 1 else 0
    holding, spare = [largest] + [least] * (amount - 1), total - largest - least * (amount - 1)
    while spare > 0:
        movable = [i for i in range(1, amount) if holding[i] < largest] or [i for i in range(1, amount) if holding[i] < reach]
        whole, budget = sum([loads[i] for i in movable]), spare
        for i in movable:
            extra = min(reach - holding[i], max(1, budget * loads[i] // whole), spare)
            holding[i] = holding[i] + extra
            spare = spare - extra
    return np.array(holding)


def gaussian(key, dims, spread, most, cuts=(), held_as=jnp.bfloat16):
    values = spread * jax.random.normal(key, dims, jnp.float32)
    if cuts:
        values = values * block_scale(key, dims, cuts, -0.22, 0.18)
    return jnp.clip(values, -most, most).astype(held_as)


def setup_inputs(seed: int = 0) -> dict:
    splits = jax.random.split(jax.random.key(seed), 18)
    tokens_first = gaussian(splits[0], (TOKENS_A, D), 1.0, 6.0, ((0, 8),))
    norm_gain_first = jnp.clip(1.0 + 0.18 * jax.random.normal(splits[1], (D,), jnp.float32), 0.1, 1.9)
    w_query = gaussian(splits[2], (D, QK_WIDTH), D ** -0.5, 0.125, ((1, 4),))
    w_key = gaussian(splits[3], (D, QK_WIDTH), D ** -0.5, 0.125, ((1, 4),))
    w_value = gaussian(splits[4], (D, V_WIDTH), D ** -0.5, 0.125, ((1, 4),))
    w_outgate = gaussian(splits[5], (D, V_WIDTH), D ** -0.5, 0.125, ((1, 4),))
    w_decay = draw_w_decay(jax.random.fold_in(splits[17], 71), 0)
    decay_bias = draw_decay_bias(jax.random.fold_in(splits[17], 71), 0)
    head_gain = jnp.clip(1.0 + 0.18 * jax.random.normal(splits[8], (V_WIDTH,), jnp.float32), 0.1, 1.9)
    w_mix_out = gaussian(splits[9], (V_WIDTH, D), V_WIDTH ** -0.5, 0.1875, ((0, 4),))
    tokens_second = gaussian(splits[10], (TOKENS_B, D), 1.0, 6.0, ((0, 8),))
    norm_gain_second = jnp.clip(1.0 + 0.18 * jax.random.normal(splits[11], (D,), jnp.float32), 0.1, 1.9)
    routes_keys = jax.random.split(jax.random.fold_in(splits[12], 1), TOKENS_B // ROWS_B)
    routes_turns = jax.random.permutation(jax.random.fold_in(splits[12], 3), TOKENS_B // ROWS_B)
    routes = jax.vmap(lambda own, number: shared_out(jax.random.fold_in(splits[12], 2), own, number, ROWS_B, EXPERTS, TOPK, CAP, 1))(routes_keys, routes_turns).reshape((TOKENS_B, TOPK))
    route_logits = gaussian(splits[13], (TOKENS_B, TOPK), 1.5, 8.0, ((0, 8),), jnp.float32)
    expert_gate = gaussian(splits[14], (EXPERTS, D, FFE), D ** -0.5, 0.125, ((0, 8), (2, 4)))
    expert_up = gaussian(splits[15], (EXPERTS, D, FFE), D ** -0.5, 0.125, ((0, 8), (2, 4)))
    expert_down = gaussian(splits[16], (EXPERTS, FFE, D), FFE ** -0.5, 0.109375, ((0, 8), (1, 4)))
    return dict(tokens_first=tokens_first, norm_gain_first=norm_gain_first, w_query=w_query, w_key=w_key, w_value=w_value, w_outgate=w_outgate, w_decay=w_decay, decay_bias=decay_bias, head_gain=head_gain, w_mix_out=w_mix_out, tokens_second=tokens_second, norm_gain_second=norm_gain_second, routes=routes, route_logits=route_logits, expert_gate=expert_gate, expert_up=expert_up, expert_down=expert_down)


EPS = 1e-06
TEMPER = 16.0

def rms_rows(rows_in, gain_row):
    wide_rows = rows_in.astype(jnp.float32)
    return wide_rows * lax.rsqrt(lax.optimization_barrier(jnp.mean(wide_rows * wide_rows, axis=-1, keepdims=True)) + EPS) * gain_row

def block_step(entry_state, inputs):
    queries, key_rows, value_matrix_rows, log_decay = inputs
    cumul_log = jnp.cumsum(log_decay, axis=0)
    forward_decay_rows = queries * jnp.exp(cumul_log)
    behind = key_rows * jnp.exp(-cumul_log)
    scores = jnp.einsum('thk,shk->hts', forward_decay_rows, behind, precision=lax.Precision.HIGHEST)
    block_len = queries.shape[0]
    causal = jnp.arange(block_len)[:, None] >= jnp.arange(block_len)[None, :]
    scores = jnp.where(causal[None], scores, jnp.zeros_like(scores))
    within = jnp.einsum('hts,shv->thv', scores, value_matrix_rows, precision=lax.Precision.HIGHEST)
    carried_state = jnp.einsum('azm,zmj->azj', forward_decay_rows, entry_state, precision=lax.Precision.HIGHEST)
    final_log_decay = cumul_log[-1]
    fading_factor = key_rows * jnp.exp(final_log_decay[None] - cumul_log)
    following_state = jnp.exp(final_log_decay)[:, :, None] * entry_state + jnp.einsum('drx,drm->rxm', fading_factor, value_matrix_rows, precision=lax.Precision.HIGHEST)
    return (following_state, within + carried_state)

def head_output(attended, out_gate, head_gain):
    scaled = attended * lax.rsqrt(lax.optimization_barrier(jnp.mean(attended * attended, axis=-1, keepdims=True)) + EPS)
    return (scaled.reshape(attended.shape[0], -1) * head_gain * jax.nn.silu(out_gate)).astype(jnp.bfloat16)

def reference(tokens_first, norm_gain_first, w_query, w_key, w_value, w_outgate, w_decay, decay_bias, head_gain, w_mix_out, tokens_second, norm_gain_second, routes, route_logits, expert_gate, expert_up, expert_down):
    normed = rms_rows(tokens_first, norm_gain_first).astype(jnp.bfloat16)
    queries = (jnp.dot(normed, w_query, preferred_element_type=jnp.float32) * KEY_DIM ** (-0.5)).astype(jnp.bfloat16)
    key_rows = jnp.dot(normed, w_key, preferred_element_type=jnp.float32).astype(jnp.bfloat16)
    value_matrix_rows = jnp.dot(normed, w_value, preferred_element_type=jnp.float32).astype(jnp.bfloat16)
    out_gate = jnp.dot(normed, w_outgate, preferred_element_type=jnp.float32)
    decay_pre = jnp.dot(normed, w_decay, preferred_element_type=jnp.float32).reshape(NBLK, BLOCK, QK_WIDTH) + decay_bias[:, None, :]
    log_decay = (jax.nn.log_sigmoid(decay_pre) / TEMPER).reshape(NBLK, BLOCK, HEADS, KEY_DIM)
    queries, key_rows, value_matrix_rows = lax.optimization_barrier((queries, key_rows, value_matrix_rows))
    query_wide = queries.astype(jnp.float32).reshape(NBLK, BLOCK, HEADS, KEY_DIM)
    key_wide = key_rows.astype(jnp.float32).reshape(NBLK, BLOCK, HEADS, KEY_DIM)
    value_wide = value_matrix_rows.astype(jnp.float32).reshape(NBLK, BLOCK, HEADS, VALUE_DIM)
    start_state = jnp.zeros((HEADS, KEY_DIM, VALUE_DIM), jnp.float32)
    _, attended = lax.scan(block_step, start_state, (query_wide, key_wide, value_wide, log_decay))
    attended = attended.reshape(TOKENS_A, HEADS, VALUE_DIM)
    gated_rows = head_output(attended, out_gate, head_gain)
    mixed_first = jnp.dot(gated_rows, w_mix_out, preferred_element_type=jnp.float32).astype(jnp.bfloat16)
    normed_second = rms_rows(tokens_second, norm_gain_second).astype(jnp.bfloat16)
    flat_routes = routes.reshape(-1)
    copies = flat_routes.shape[0]
    slot_room = N_EP * CAP

    def expert_rows(expert_id, collected):
        copy_index = jnp.nonzero(flat_routes == expert_id, size=slot_room, fill_value=copies)[0]
        picked_rows = jnp.take(normed_second, copy_index // TOPK, axis=0, mode='clip')
        gate_out = jnp.dot(picked_rows, expert_gate[expert_id], preferred_element_type=jnp.float32)
        up_out = jnp.dot(picked_rows, expert_up[expert_id], preferred_element_type=jnp.float32)
        hidden = (jax.nn.silu(gate_out) * up_out).astype(jnp.bfloat16)
        hidden_wide = hidden.reshape(slot_room, N_TP, FFE // N_TP).astype(jnp.float32)
        down_wide = expert_down[expert_id].reshape(N_TP, FFE // N_TP, D).astype(jnp.float32)
        tp_parts = jnp.einsum('mtf,tfd->tmd', hidden_wide, down_wide).astype(jnp.bfloat16)
        tp_parts = lax.optimization_barrier(tp_parts).astype(jnp.float32)
        result = lax.optimization_barrier(jnp.sum(tp_parts, axis=0)).astype(jnp.bfloat16)
        return collected.at[copy_index].set(result, mode='drop')
    collected = lax.fori_loop(0, EXPERTS, expert_rows, jnp.zeros((copies, D), jnp.bfloat16))
    route_share = jax.nn.sigmoid(route_logits - route_logits[:, ::-1])
    picked = collected.reshape(TOKENS_B, TOPK, D).astype(jnp.float32)
    mixed_second = lax.optimization_barrier(jnp.sum(picked * route_share[:, :, None], axis=1)).astype(jnp.bfloat16)
    return (mixed_first, mixed_second)
```

```python
import functools

import jax
import jax.numpy as jnp
from jax import lax
from jax.experimental import pallas as pl
from jax.experimental.pallas import tpu as pltpu
from jax.sharding import PartitionSpec as P

KEY_DIM = 64
VALUE_DIM = 128
BLOCK = 64
EPS = 1e-06
TEMPER = 16.0
CHUNKS = 4
LANES = 128

MESH = pl.DeviceIdType.MESH
F32 = jnp.float32
BF16 = jnp.bfloat16


def flip(index, mask):
    bit = 1
    while bit <= mask:
        if mask & bit:
            index = index + bit - 2 * bit * ((index // bit) % 2)
        bit *= 2
    return index


def dot(a, b):
    return jnp.dot(a, b, preferred_element_type=F32)


def dot_t(a, b, dims):
    return lax.dot_general(a, b, (dims, ((), ())), preferred_element_type=F32)


def rms_scale(wide):
    return lax.rsqrt(jnp.mean(wide * wide, axis=-1, keepdims=True) + EPS)


def kernel(
    n_ep,
    n_tp,
    tokens_first,
    gain_first,
    w_query,
    w_key,
    w_value,
    w_outgate,
    w_decay,
    decay_bias,
    head_gain,
    w_mix_out,
    tokens_second,
    gain_second,
    routes,
    routes_t,
    logits,
    e_gate,
    e_up,
    e_down,
    out_first,
    out_second,
    tf,
    wq,
    wk,
    wv,
    wg,
    wd,
    wm,
    ts,
    eg,
    eu,
    ed,
    normed,
    q_s,
    k_s,
    v_s,
    g_s,
    cum_s,
    state_s,
    st_send,
    fade_send,
    st_recv,
    fade_recv,
    inc,
    gated,
    mixp,
    mrecv1,
    msend,
    mrecv2,
    slots,
    rows,
    hid,
    part,
    recv1,
    send2,
    recv2,
    result,
    received,
    load_sem,
    disp_ss,
    disp_rs,
    xf_ss,
    xf_rs,
    cf_ss,
    cf_rs,
    st_ss,
    st_rs,
    fd_ss,
    fd_rs,
    m1_ss,
    m1_rs,
    m2_ss,
    m2_rs,
    r1_ss,
    r1_rs,
    r2_ss,
    r2_rs,
    ret_ss,
    ret_rs,
):
    e = lax.axis_index("ep")
    t = lax.axis_index("tp")
    lo = t % 2
    hi = t // 2
    near = flip(t, 1)
    far = flip(t, 2)
    cross = flip(t, 3)
    hi_other = 1 - hi

    loads = [
        pltpu.make_async_copy(src, dst, load_sem.at[i])
        for i, (src, dst) in enumerate(
            [
                (tokens_second, ts),
                (tokens_first, tf),
                (w_query, wq),
                (w_key, wk),
                (w_decay, wd),
                (w_value, wv),
                (w_outgate, wg),
                (e_gate, eg),
                (e_up, eu),
                (e_down, ed),
                (w_mix_out, wm),
            ]
        )
    ]
    for load in loads:
        load.start()

    barrier = pltpu.get_barrier_semaphore()
    for j in range(1, n_ep):
        pl.semaphore_signal(barrier, inc=1, device_id=(flip(e, j), t), device_id_type=MESH)
    for peer in (near, far):
        pl.semaphore_signal(barrier, inc=1, device_id=(e, peer), device_id_type=MESH)

    n_rows = ts.shape[0]
    n_slots, width = slots.shape
    room = n_slots // n_ep
    expert_col = lax.broadcasted_iota(jnp.int32, (LANES, n_rows), 0)
    rt = routes_t[...]
    m0 = (expert_col == rt[0:1, :]).astype(F32)
    m1 = (expert_col == rt[1:2, :]).astype(F32)
    r_i = lax.broadcasted_iota(jnp.int32, (n_rows, n_rows), 0)
    c_i = lax.broadcasted_iota(jnp.int32, (n_rows, n_rows), 1)
    before = dot((m0 + m1).astype(BF16), (r_i < c_i).astype(BF16))
    t0 = rt[0:1, :] * room + jnp.sum(m0 * before, axis=0, keepdims=True).astype(jnp.int32)
    t1 = rt[1:2, :] * room + jnp.sum(m1 * before, axis=0, keepdims=True).astype(jnp.int32)
    loads[0].wait()
    scale2 = rms_scale(ts[...].astype(F32))
    mine = pl.ds(pl.multiple_of(t * width, width), width)
    piece = (ts[:, mine].astype(F32) * scale2 * gain_second[:, mine]).astype(BF16)

    def build(i, carry):
        start = pl.multiple_of(i * 256, 256)
        slot_id = lax.broadcasted_iota(jnp.int32, (256, n_rows), 0) + start
        pick = ((slot_id == t0) | (slot_id == t1)).astype(F32).astype(BF16)
        slots[pl.ds(start, 256), :] = dot(pick, piece).astype(BF16)
        return carry

    lax.fori_loop(0, n_slots // 256, build, 0)

    def place(s):
        return pl.ds(pl.multiple_of(s * room, room), room)

    pl.semaphore_wait(barrier, n_ep + 1)

    def remote(src, dst, ss, rs, dev):
        return pltpu.make_async_remote_copy(
            src_ref=src, dst_ref=dst, send_sem=ss, recv_sem=rs, device_id=dev, device_id_type=MESH
        )

    disp = [None]
    for j in range(1, n_ep):
        s = flip(e, j)
        disp.append(
            remote(
                slots.at[place(s), :], rows.at[t, place(e), :], disp_ss.at[j], disp_rs.at[j], (s, t)
            )
        )
        disp[j].start()
    rows[t, place(e), :] = slots[place(e), :]

    xf, cf0, cf1 = [], [], []
    for j in range(n_ep):
        p = place(flip(e, j))
        xf.append(remote(rows.at[t, p, :], rows.at[t, p, :], xf_ss.at[j], xf_rs.at[j], (e, far)))
        cf0.append(
            remote(rows.at[t, p, :], rows.at[t, p, :], cf_ss.at[j, 0], cf_rs.at[j, 0], (e, near))
        )
        cf1.append(
            remote(
                rows.at[far, p, :], rows.at[far, p, :], cf_ss.at[j, 1], cf_rs.at[j, 1], (e, near)
            )
        )
    per_chunk = n_ep // CHUNKS

    def forward_own(c):
        for j in range(c * per_chunk, (c + 1) * per_chunk):
            if j > 0:
                disp[j].wait_recv()
            xf[j].start()
            cf0[j].start()

    def forward_far(c):
        for j in range(c * per_chunk, (c + 1) * per_chunk):
            xf[j].wait_recv()
            cf1[j].start()

    def arrived(c):
        for j in range(c * per_chunk, (c + 1) * per_chunk):
            cf0[j].wait_recv()
            cf1[j].wait_recv()

    xf[0].start()
    cf0[0].start()

    loads[1].wait()
    n_first = tf.shape[0]
    blocks = n_first // BLOCK

    def norm_rows(i, carry):
        at = pl.ds(pl.multiple_of(i * BLOCK, BLOCK), BLOCK)
        wide = tf[at, :].astype(F32)
        normed[at, :] = (wide * rms_scale(wide) * gain_first[...]).astype(BF16)
        return carry

    lax.fori_loop(0, blocks, norm_rows, 0)
    loads[2].wait()
    q_s[...] = (dot(normed[...], wq[...]) * KEY_DIM ** (-0.5)).astype(BF16)
    loads[3].wait()
    k_s[...] = dot(normed[...], wk[...]).astype(BF16)
    loads[4].wait()
    cum_s[...] = dot(normed[...], wd[...])
    for j in range(1, per_chunk):
        disp[j].wait_recv()
        xf[j].start()
        cf0[j].start()
    loads[5].wait()
    v_s[...] = dot(normed[...], wv[...]).astype(BF16)
    loads[6].wait()
    g_s[...] = dot(normed[...], wg[...])
    forward_own(1)
    forward_far(0)

    keys = k_s.shape[1]
    heads = keys // KEY_DIM
    tri_r = lax.broadcasted_iota(jnp.int32, (BLOCK, BLOCK), 0)
    tri_c = lax.broadcasted_iota(jnp.int32, (BLOCK, BLOCK), 1)
    causal = tri_r >= tri_c
    tri = causal.astype(F32)
    head_of = lax.broadcasted_iota(jnp.int32, (1, keys), 1) // KEY_DIM
    inc[...] = jnp.zeros_like(inc)

    def local_pass(b, total):
        at = pl.ds(pl.multiple_of(b * BLOCK, BLOCK), BLOCK)
        pre = cum_s[at, :] + decay_bias[pl.ds(b, 1), :]
        log_decay = (jnp.minimum(pre, 0.0) - jnp.log1p(jnp.exp(-jnp.abs(pre)))) / TEMPER
        cum = jnp.dot(tri, log_decay, precision=lax.Precision.HIGHEST, preferred_element_type=F32)
        cum_s[at, :] = cum
        last = cum[BLOCK - 1 : BLOCK, :]
        fading = (k_s[at, :].astype(F32) * jnp.exp(last - cum)).astype(BF16)
        full = dot_t(v_s[at, :], fading, ((0,), (0,)))
        add = full[0:VALUE_DIM]
        for h in range(1, heads):
            add = jnp.where(head_of == h, full[h * VALUE_DIM : (h + 1) * VALUE_DIM], add)
        state_s[b] = inc[...]
        inc[...] = inc[...] * jnp.exp(last) + add
        return total + last

    total = lax.fori_loop(0, blocks, local_pass, jnp.zeros((1, keys), F32))
    st_send[...] = inc[...].astype(BF16)
    fade_send[...] = jnp.broadcast_to(jnp.exp(total), fade_send.shape)

    def state_copies(k, dst):
        return (
            remote(st_send, st_recv.at[k], st_ss.at[k], st_rs.at[k], (dst, t)),
            remote(fade_send, fade_recv.at[k], fd_ss.at[k], fd_rs.at[k], (dst, t)),
        )

    for k in range(1, n_ep):

        @pl.when(e + k < n_ep)
        def _():
            for copy in state_copies(k, e + k):
                copy.start()

    chunk_rows = n_slots // CHUNKS
    hidden_width = hid.shape[1]
    tile = 256

    def chunk_at(c):
        m = flip(e // per_chunk, c)
        return pl.ds(pl.multiple_of(m * chunk_rows, chunk_rows), chunk_rows)

    def experts(c):
        at = chunk_at(c)

        def up(i, carry):
            cols = pl.ds(pl.multiple_of(i * tile, tile), tile)
            gate = jnp.zeros((chunk_rows, tile), F32)
            upper = jnp.zeros((chunk_rows, tile), F32)
            for b in range(n_tp):
                x = rows[b, at, :]
                gate = gate + dot(x, eg[0, b * width : (b + 1) * width, cols])
                upper = upper + dot(x, eu[0, b * width : (b + 1) * width, cols])
            hid[:, cols] = (gate * jax.nn.sigmoid(gate) * upper).astype(BF16)
            return carry

        lax.fori_loop(0, hidden_width // tile, up, 0)

        def down(b, carry):
            cols = pl.ds(pl.multiple_of(b * width, width), width)
            part[b, at, :] = dot(hid[...], ed[0, :, cols]).astype(BF16)
            return carry

        lax.fori_loop(0, n_tp, down, 0)

    near_lo = 1 - lo
    r1, r2, ret = [], [], []
    for c in range(CHUNKS):
        at = chunk_at(c)
        r1.append(
            [
                remote(
                    part.at[2 * h + near_lo, at, :],
                    recv1.at[h, at, :],
                    r1_ss.at[c, h],
                    r1_rs.at[c, h],
                    (e, near),
                )
                for h in range(2)
            ]
        )
        r2.append(remote(send2.at[at, :], recv2.at[at, :], r2_ss.at[c], r2_rs.at[c], (e, far)))
    for j in range(n_ep):
        s = flip(e, j)
        ret.append(
            remote(
                result.at[place(s), :], received.at[place(e), :], ret_ss.at[j], ret_rs.at[j], (s, t)
            )
        )

    def send_near(c):
        for copy in r1[c]:
            copy.start()

    def send_far(c):
        at = chunk_at(c)
        for copy in r1[c]:
            copy.wait_recv()
        send2[at, :] = (
            part[2 * hi_other + lo, at, :].astype(F32) + recv1[hi_other, at, :].astype(F32)
        ).astype(BF16)
        r2[c].start()

    def send_back(c):
        at = chunk_at(c)
        r2[c].wait_recv()
        result[at, :] = (
            part[t, at, :].astype(F32)
            + recv1[hi, at, :].astype(F32)
            + recv2[at, :].astype(F32)
        ).astype(BF16)
        for j in range(c * per_chunk, (c + 1) * per_chunk):
            if j > 0:
                ret[j].start()
        if c == 0:
            received[place(e), :] = result[place(e), :]

    forward_own(2)
    forward_far(1)
    for load in loads[7:10]:
        load.wait()
    arrived(0)
    experts(0)
    send_near(0)
    forward_own(3)
    forward_far(2)
    arrived(1)
    experts(1)
    send_near(1)
    send_far(0)
    forward_far(3)
    arrived(2)
    experts(2)
    send_near(2)
    send_far(1)
    send_back(0)
    arrived(3)
    experts(3)
    send_near(3)
    send_far(2)
    send_back(1)

    inc[...] = jnp.zeros_like(inc)
    for k in range(n_ep - 1, 0, -1):

        @pl.when(e >= k)
        def _():
            for copy in state_copies(k, e):
                copy.wait_recv()
            inc[...] = inc[...] * fade_recv[k, 0:1, :] + st_recv[k].astype(F32)

    def final_pass(b, before_log):
        at = pl.ds(pl.multiple_of(b * BLOCK, BLOCK), BLOCK)
        cum = cum_s[at, :]
        ahead = (q_s[at, :].astype(F32) * jnp.exp(cum)).astype(BF16)
        behind = (k_s[at, :].astype(F32) * jnp.exp(-cum)).astype(BF16)
        entry = (state_s[b] + inc[...] * jnp.exp(before_log)).astype(BF16)
        for h in range(heads):
            cols = slice(h * VALUE_DIM, (h + 1) * VALUE_DIM)
            own = jnp.where(head_of == h, ahead, jnp.zeros_like(ahead))
            scores = jnp.where(causal, dot_t(own, behind, ((1,), (1,))), 0.0)
            attended = dot(scores.astype(BF16), v_s[at, cols]) + dot_t(own, entry, ((1,), (1,)))
            gate = g_s[at, cols]
            gated[at, cols] = (
                attended
                * rms_scale(attended)
                * head_gain[:, cols]
                * (gate * jax.nn.sigmoid(gate))
            ).astype(BF16)
        return before_log + cum[BLOCK - 1 : BLOCK, :]

    lax.fori_loop(0, blocks, final_pass, jnp.zeros((1, keys), F32))
    loads[10].wait()
    mix_rows = n_first // n_tp

    def mix(i, carry):
        at = pl.ds(pl.multiple_of(i * mix_rows, mix_rows), mix_rows)
        mixp[i] = dot(gated[at, :], wm[...]).astype(BF16)
        return carry

    lax.fori_loop(0, n_tp, mix, 0)
    mix1 = [
        remote(
            mixp.at[2 * h + near_lo], mrecv1.at[h], m1_ss.at[h], m1_rs.at[h], (e, near)
        )
        for h in range(2)
    ]
    for copy in mix1:
        copy.start()
    send_far(3)
    send_back(2)
    for copy in mix1:
        copy.wait_recv()
    msend[...] = (
        mixp[2 * hi_other + lo].astype(F32) + mrecv1[hi_other].astype(F32)
    ).astype(BF16)
    mix2 = remote(msend, mrecv2, m2_ss.at[0], m2_rs.at[0], (e, far))
    mix2.start()
    send_back(3)
    mix2.wait_recv()
    out_first[...] = (
        mixp[t].astype(F32) + mrecv1[hi].astype(F32) + mrecv2[...].astype(F32)
    ).astype(BF16)

    col_expert = lax.broadcasted_iota(jnp.int32, (n_rows, LANES), 1)
    route = routes[...]
    n0 = (col_expert == route[:, 0:1]).astype(F32)
    n1 = (col_expert == route[:, 1:2]).astype(F32)
    ahead_of = dot((r_i > c_i).astype(BF16), (n0 + n1).astype(BF16))
    u0 = route[:, 0:1] * room + jnp.sum(n0 * ahead_of, axis=1, keepdims=True).astype(jnp.int32)
    u1 = route[:, 1:2] * room + jnp.sum(n1 * ahead_of, axis=1, keepdims=True).astype(jnp.int32)
    log0 = logits[:, 0:1]
    log1 = logits[:, 1:2]
    slot_col = lax.broadcasted_iota(jnp.int32, (n_rows, n_slots), 1)
    pick0 = (slot_col == u0).astype(F32).astype(BF16)
    pick1 = (slot_col == u1).astype(F32).astype(BF16)
    for j in range(1, n_ep):
        ret[j].wait_recv()
    out_second[...] = (
        dot(pick0, received[...]) * jax.nn.sigmoid(log0 - log1)
        + dot(pick1, received[...]) * jax.nn.sigmoid(log1 - log0)
    ).astype(BF16)

    for j in range(n_ep):
        if j > 0:
            disp[j].wait_send()
            ret[j].wait_send()
        xf[j].wait_send()
        cf0[j].wait_send()
        cf1[j].wait_send()
    for c in range(CHUNKS):
        for copy in r1[c]:
            copy.wait_send()
        r2[c].wait_send()
    for copy in mix1:
        copy.wait_send()
    mix2.wait_send()
    for k in range(1, n_ep):

        @pl.when(e + k < n_ep)
        def _():
            for copy in state_copies(k, e + k):
                copy.wait_send()


def body(
    tokens_first,
    norm_gain_first,
    w_query,
    w_key,
    w_value,
    w_outgate,
    w_decay,
    decay_bias,
    head_gain,
    w_mix_out,
    tokens_second,
    norm_gain_second,
    routes,
    route_logits,
    expert_gate,
    expert_up,
    expert_down,
):
    n_ep = lax.axis_size("ep")
    n_tp = lax.axis_size("tp")
    n_first, model = tokens_first.shape
    n_rows = tokens_second.shape[0]
    room = 2 * routes.shape[1] * n_rows // (n_ep * expert_gate.shape[0])
    n_slots = n_ep * room
    width = model // n_tp
    keys = w_query.shape[1]
    values = w_value.shape[1]
    hidden = expert_gate.shape[2]
    blocks = n_first // BLOCK
    mix_rows = n_first // n_tp
    chunk_rows = n_slots // CHUNKS
    vmem = pltpu.VMEM
    dma = pltpu.SemaphoreType.DMA

    def like(x):
        return vmem(x.shape, x.dtype)

    whole = pl.BlockSpec(memory_space=pltpu.VMEM)
    away = pl.BlockSpec(memory_space=pl.ANY)
    scratch = [
        like(tokens_first),
        like(w_query),
        like(w_key),
        like(w_value),
        like(w_outgate),
        like(w_decay),
        like(w_mix_out),
        like(tokens_second),
        like(expert_gate),
        like(expert_up),
        like(expert_down),
        vmem((n_first, model), BF16),
        vmem((n_first, keys), BF16),
        vmem((n_first, keys), BF16),
        vmem((n_first, values), BF16),
        vmem((n_first, values), F32),
        vmem((n_first, keys), F32),
        vmem((blocks, VALUE_DIM, keys), F32),
        vmem((VALUE_DIM, keys), BF16),
        vmem((8, keys), F32),
        vmem((n_ep, VALUE_DIM, keys), BF16),
        vmem((n_ep, 8, keys), F32),
        vmem((VALUE_DIM, keys), F32),
        vmem((n_first, values), BF16),
        vmem((n_tp, mix_rows, model), BF16),
        vmem((2, mix_rows, model), BF16),
        vmem((mix_rows, model), BF16),
        vmem((mix_rows, model), BF16),
        vmem((n_slots, width), BF16),
        vmem((n_tp, n_slots, width), BF16),
        vmem((chunk_rows, hidden), BF16),
        vmem((n_tp, n_slots, width), BF16),
        vmem((2, n_slots, width), BF16),
        vmem((n_slots, width), BF16),
        vmem((n_slots, width), BF16),
        vmem((n_slots, width), BF16),
        vmem((n_slots, width), BF16),
        dma((11,)),
        dma((n_ep,)),
        dma((n_ep,)),
        dma((n_ep,)),
        dma((n_ep,)),
        dma((n_ep, 2)),
        dma((n_ep, 2)),
        dma((n_ep,)),
        dma((n_ep,)),
        dma((n_ep,)),
        dma((n_ep,)),
        dma((2,)),
        dma((2,)),
        dma((1,)),
        dma((1,)),
        dma((CHUNKS, 2)),
        dma((CHUNKS, 2)),
        dma((CHUNKS,)),
        dma((CHUNKS,)),
        dma((n_ep,)),
        dma((n_ep,)),
    ]
    return pl.pallas_call(
        functools.partial(kernel, n_ep, n_tp),
        out_shape=(
            jax.ShapeDtypeStruct((mix_rows, model), BF16),
            jax.ShapeDtypeStruct((n_rows, width), BF16),
        ),
        in_specs=[away, whole, away, away, away, away, away, whole, whole, away]
        + [away, whole, whole, whole, whole, away, away, away],
        out_specs=(whole, whole),
        scratch_shapes=scratch,
        compiler_params=pltpu.CompilerParams(
            collective_id=0, has_side_effects=True, vmem_limit_bytes=60 * 1024 * 1024
        ),
    )(
        tokens_first,
        norm_gain_first[None, :],
        w_query,
        w_key,
        w_value,
        w_outgate,
        w_decay,
        decay_bias,
        head_gain[None, :],
        w_mix_out,
        tokens_second,
        norm_gain_second[None, :],
        routes,
        routes.T,
        route_logits,
        expert_gate,
        expert_up,
        expert_down,
    )


def solution(mesh):
    in_specs = (
        P("ep", None),
        P(),
        P(None, "tp"),
        P(None, "tp"),
        P(None, "tp"),
        P(None, "tp"),
        P(None, "tp"),
        P("ep", "tp"),
        P("tp"),
        P("tp", None),
        P("ep", None),
        P(),
        P("ep", None),
        P("ep", None),
        P("ep", None, "tp"),
        P("ep", None, "tp"),
        P("ep", "tp", None),
    )
    out_specs = (P(("ep", "tp"), None), P("ep", "tp"))
    return jax.shard_map(body, mesh=mesh, in_specs=in_specs, out_specs=out_specs, check_vma=False)
```

```python
import functools

import jax
import jax.numpy as jnp
from jax import lax
from jax.experimental import pallas as pl
from jax.experimental.pallas import tpu as pltpu
from jax.sharding import PartitionSpec as P

KEY_DIM = 64
VALUE_DIM = 128
BLOCK = 64
EPS = 1e-06
TEMPER = 16.0
CHUNKS = 4
LANES = 128

MESH = pl.DeviceIdType.MESH
F32 = jnp.float32
BF16 = jnp.bfloat16


def flip(index, mask):
    bit = 1
    while bit <= mask:
        if mask & bit:
            index = index + bit - 2 * bit * ((index // bit) % 2)
        bit *= 2
    return index


def dot(a, b):
    return jnp.dot(a, b, preferred_element_type=F32)


def dot_t(a, b, dims):
    return lax.dot_general(a, b, (dims, ((), ())), preferred_element_type=F32)


def rms_scale(wide):
    return lax.rsqrt(jnp.mean(wide * wide, axis=-1, keepdims=True) + EPS)


def kernel(
    n_ep,
    n_tp,
    tokens_first,
    gain_first,
    w_query,
    w_key,
    w_value,
    w_outgate,
    w_decay,
    decay_bias,
    head_gain,
    w_mix_out,
    tokens_second,
    gain_second,
    routes_t,
    logits_t,
    e_gate,
    e_up,
    e_down,
    out_first,
    out_second,
    tf,
    wq,
    wk,
    wv,
    wg,
    wd,
    wm,
    ts,
    eg,
    eu,
    ed,
    normed,
    q_s,
    k_s,
    v_s,
    g_s,
    cum_s,
    state_s,
    st_send,
    fade_send,
    st_recv,
    fade_recv,
    inc,
    gated,
    mixp,
    mrecv1,
    msend,
    mrecv2,
    slots,
    rows,
    hid,
    part,
    recv1,
    send2,
    recv2,
    result,
    received,
    picks,
    load_sem,
    disp_ss,
    disp_rs,
    dup_ss,
    dup_rs,
    xf_ss,
    xf_rs,
    cf_ss,
    cf_rs,
    st_ss,
    st_rs,
    fd_ss,
    fd_rs,
    m1_ss,
    m1_rs,
    m2_ss,
    m2_rs,
    r1_ss,
    r1_rs,
    r2_ss,
    r2_rs,
    ret_ss,
    ret_rs,
):
    e = lax.axis_index("ep")
    t = lax.axis_index("tp")
    lo = t % 2
    hi = t // 2
    near = flip(t, 1)
    far = flip(t, 2)
    cross = flip(t, 3)
    hi_other = 1 - hi

    loads = [
        pltpu.make_async_copy(src, dst, load_sem.at[i])
        for i, (src, dst) in enumerate(
            [
                (tokens_second, ts),
                (tokens_first, tf),
                (w_query, wq),
                (w_key, wk),
                (w_decay, wd),
                (w_value, wv),
                (w_outgate, wg),
                (e_gate, eg),
                (e_up, eu),
                (e_down, ed),
                (w_mix_out, wm),
            ]
        )
    ]
    for load in loads:
        load.start()

    barrier = pltpu.get_barrier_semaphore()
    for j in range(1, n_ep):
        pl.semaphore_signal(barrier, inc=1, device_id=(flip(e, j), t), device_id_type=MESH)
    for peer in (near, far):
        pl.semaphore_signal(barrier, inc=1, device_id=(e, peer), device_id_type=MESH)

    n_rows = ts.shape[0]
    _, n_slots, width = slots.shape
    room = n_slots // n_ep
    expert_col = lax.broadcasted_iota(jnp.int32, (LANES, n_rows), 0)
    rt = routes_t[...]
    m0 = (expert_col == rt[0:1, :]).astype(F32)
    m1 = (expert_col == rt[1:2, :]).astype(F32)
    r_i = lax.broadcasted_iota(jnp.int32, (n_rows, n_rows), 0)
    c_i = lax.broadcasted_iota(jnp.int32, (n_rows, n_rows), 1)
    before = dot((m0 + m1).astype(BF16), (r_i < c_i).astype(BF16))
    t0 = rt[0:1, :] * room + jnp.sum(m0 * before, axis=0, keepdims=True).astype(jnp.int32)
    t1 = rt[1:2, :] * room + jnp.sum(m1 * before, axis=0, keepdims=True).astype(jnp.int32)
    loads[0].wait()
    scale2 = rms_scale(ts[...].astype(F32))

    def features(block):
        cols = pl.ds(pl.multiple_of(block * width, width), width)
        return (ts[:, cols].astype(F32) * scale2 * gain_second[:, cols]).astype(BF16)

    def chosen(start, count):
        slot_id = lax.broadcasted_iota(jnp.int32, (count, n_rows), 0) + start
        return ((slot_id == t0) | (slot_id == t1)).astype(F32).astype(BF16)

    pieces = (features(t), features(far))

    def build(i, carry):
        start = pl.multiple_of(i * 256, 256)
        pick = chosen(start, 256)
        for which in range(2):
            slots[which, pl.ds(start, 256), :] = dot(pick, pieces[which]).astype(BF16)
        return carry

    lax.fori_loop(0, n_slots // 256, build, 0)

    def place(s):
        return pl.ds(pl.multiple_of(s * room, room), room)

    pl.semaphore_wait(barrier, n_ep + 1)

    def remote(src, dst, ss, rs, dev):
        return pltpu.make_async_remote_copy(
            src_ref=src, dst_ref=dst, send_sem=ss, recv_sem=rs, device_id=dev, device_id_type=MESH
        )

    per_chunk = n_ep // CHUNKS

    def members(c):
        return list(range(c * per_chunk, (c + 1) * per_chunk))

    doubled = 2 * per_chunk
    disp, dup = [None], [None]
    for j in range(1, n_ep):
        s = flip(e, j)
        disp.append(
            remote(
                slots.at[0, place(s), :],
                rows.at[t, place(e), :],
                disp_ss.at[j],
                disp_rs.at[j],
                (s, t),
            )
        )
        if j < doubled:
            dup.append(
                remote(
                    slots.at[1, place(s), :],
                    rows.at[far, place(e), :],
                    dup_ss.at[j],
                    dup_rs.at[j],
                    (s, t),
                )
            )

    def dispatch(j):
        disp[j].start()
        if j < doubled:
            dup[j].start()

    half_chunk = per_chunk // 2
    early = members(0)[1:] + members(2) + members(3)[:half_chunk]
    late = members(3)[half_chunk:] + members(1)
    for j in early:
        dispatch(j)
    own_pick = chosen(e * room, room)
    rows[t, place(e), :] = slots[0, place(e), :]
    rows[far, place(e), :] = slots[1, place(e), :]
    rows[near, place(e), :] = dot(own_pick, features(near)).astype(BF16)
    rows[cross, place(e), :] = dot(own_pick, features(cross)).astype(BF16)

    xf, cf0, cf1 = [], [], []
    for j in range(n_ep):
        p = place(flip(e, j))
        xf.append(
            None
            if j < doubled
            else remote(rows.at[t, p, :], rows.at[t, p, :], xf_ss.at[j], xf_rs.at[j], (e, far))
        )
        cf0.append(
            None
            if j == 0
            else remote(
                rows.at[t, p, :], rows.at[t, p, :], cf_ss.at[j, 0], cf_rs.at[j, 0], (e, near)
            )
        )
        cf1.append(
            None
            if j == 0
            else remote(
                rows.at[far, p, :], rows.at[far, p, :], cf_ss.at[j, 1], cf_rs.at[j, 1], (e, near)
            )
        )

    def forward_own(js):
        for j in js:
            if j > 0:
                disp[j].wait_recv()
                if j >= doubled:
                    xf[j].start()
                cf0[j].start()

    def forward_far(js):
        for j in js:
            if j > 0:
                if j < doubled:
                    dup[j].wait_recv()
                else:
                    xf[j].wait_recv()
                cf1[j].start()

    def arrived(c):
        for j in members(c):
            if j > 0:
                cf0[j].wait_recv()
                cf1[j].wait_recv()

    loads[1].wait()
    n_first = tf.shape[0]
    blocks = n_first // BLOCK

    def norm_rows(i, carry):
        at = pl.ds(pl.multiple_of(i * BLOCK, BLOCK), BLOCK)
        wide = tf[at, :].astype(F32)
        normed[at, :] = (wide * rms_scale(wide) * gain_first[...]).astype(BF16)
        return carry

    lax.fori_loop(0, blocks, norm_rows, 0)
    loads[2].wait()
    q_s[...] = (dot(normed[...], wq[...]) * KEY_DIM ** (-0.5)).astype(BF16)
    loads[3].wait()
    k_s[...] = dot(normed[...], wk[...]).astype(BF16)
    loads[4].wait()
    cum_s[...] = dot(normed[...], wd[...])
    loads[5].wait()
    v_s[...] = dot(normed[...], wv[...]).astype(BF16)
    loads[6].wait()
    g_s[...] = dot(normed[...], wg[...])

    keys = k_s.shape[1]
    heads = keys // KEY_DIM
    tri_r = lax.broadcasted_iota(jnp.int32, (BLOCK, BLOCK), 0)
    tri_c = lax.broadcasted_iota(jnp.int32, (BLOCK, BLOCK), 1)
    causal = tri_r >= tri_c
    tri = causal.astype(F32)
    head_of = lax.broadcasted_iota(jnp.int32, (1, keys), 1) // KEY_DIM
    inc[...] = jnp.zeros_like(inc)

    def local_pass(b, total):
        at = pl.ds(pl.multiple_of(b * BLOCK, BLOCK), BLOCK)
        pre = cum_s[at, :] + decay_bias[pl.ds(b, 1), :]
        log_decay = (jnp.minimum(pre, 0.0) - jnp.log1p(jnp.exp(-jnp.abs(pre)))) / TEMPER
        cum = jnp.dot(tri, log_decay, precision=lax.Precision.HIGHEST, preferred_element_type=F32)
        cum_s[at, :] = cum
        last = cum[BLOCK - 1 : BLOCK, :]
        fading = (k_s[at, :].astype(F32) * jnp.exp(last - cum)).astype(BF16)
        full = dot_t(v_s[at, :], fading, ((0,), (0,)))
        add = full[0:VALUE_DIM]
        for h in range(1, heads):
            add = jnp.where(head_of == h, full[h * VALUE_DIM : (h + 1) * VALUE_DIM], add)
        state_s[b] = inc[...]
        inc[...] = inc[...] * jnp.exp(last) + add
        return total + last

    total = lax.fori_loop(0, blocks, local_pass, jnp.zeros((1, keys), F32))
    st_send[...] = inc[...].astype(BF16)
    fade_send[...] = jnp.broadcast_to(jnp.exp(total), fade_send.shape)

    def state_copies(k, dst):
        return (
            remote(st_send, st_recv.at[k], st_ss.at[k], st_rs.at[k], (dst, t)),
            remote(fade_send, fade_recv.at[k], fd_ss.at[k], fd_rs.at[k], (dst, t)),
        )

    for k in range(1, n_ep):

        @pl.when(e + k < n_ep)
        def _():
            for copy in state_copies(k, e + k):
                copy.start()

    for j in late:
        dispatch(j)

    chunk_rows = n_slots // CHUNKS
    hidden_width = hid.shape[1]
    tile = 256

    def chunk_at(c):
        m = flip(e // per_chunk, c)
        return pl.ds(pl.multiple_of(m * chunk_rows, chunk_rows), chunk_rows)

    def experts(c):
        at = chunk_at(c)

        def up(i, carry):
            cols = pl.ds(pl.multiple_of(i * tile, tile), tile)
            gate = jnp.zeros((chunk_rows, tile), F32)
            upper = jnp.zeros((chunk_rows, tile), F32)
            for b in range(n_tp):
                x = rows[b, at, :]
                gate = gate + dot(x, eg[0, b * width : (b + 1) * width, cols])
                upper = upper + dot(x, eu[0, b * width : (b + 1) * width, cols])
            hid[:, cols] = (gate * jax.nn.sigmoid(gate) * upper).astype(BF16)
            return carry

        lax.fori_loop(0, hidden_width // tile, up, 0)

        def down(b, carry):
            cols = pl.ds(pl.multiple_of(b * width, width), width)
            part[b, at, :] = dot(hid[...], ed[0, :, cols]).astype(BF16)
            return carry

        lax.fori_loop(0, n_tp, down, 0)

    near_lo = 1 - lo
    r1, r2, ret = [], [], []
    for c in range(CHUNKS):
        at = chunk_at(c)
        r1.append(
            [
                remote(
                    part.at[2 * h + near_lo, at, :],
                    recv1.at[h, at, :],
                    r1_ss.at[c, h],
                    r1_rs.at[c, h],
                    (e, near),
                )
                for h in range(2)
            ]
        )
        r2.append(remote(send2.at[at, :], recv2.at[at, :], r2_ss.at[c], r2_rs.at[c], (e, far)))
    for j in range(n_ep):
        s = flip(e, j)
        ret.append(
            remote(
                result.at[place(s), :], received.at[place(e), :], ret_ss.at[j], ret_rs.at[j], (s, t)
            )
        )

    def send_near(c):
        for copy in r1[c]:
            copy.start()

    def send_far(c):
        at = chunk_at(c)
        for copy in r1[c]:
            copy.wait_recv()
        send2[at, :] = (
            part[2 * hi_other + lo, at, :].astype(F32) + recv1[hi_other, at, :].astype(F32)
        ).astype(BF16)
        r2[c].start()

    def send_back(c):
        at = chunk_at(c)
        r2[c].wait_recv()
        result[at, :] = (
            part[t, at, :].astype(F32)
            + recv1[hi, at, :].astype(F32)
            + recv2[at, :].astype(F32)
        ).astype(BF16)
        for j in range(c * per_chunk, (c + 1) * per_chunk):
            if j > 0:
                ret[j].start()
        if c == 0:
            received[place(e), :] = result[place(e), :]

    share0 = jax.nn.sigmoid(logits_t[0:1, :] - logits_t[1:2, :])
    share1 = jax.nn.sigmoid(logits_t[1:2, :] - logits_t[0:1, :])
    stacked = jnp.concatenate(
        [
            t0.astype(F32),
            t1.astype(F32),
            share0,
            share1,
            jnp.zeros((LANES - 4, n_rows), F32),
        ],
        axis=0,
    )
    columns = jnp.transpose(stacked)
    slot_col = lax.broadcasted_iota(jnp.int32, (n_rows, n_slots), 1)
    for which in range(2):
        at_slot = columns[:, which : which + 1].astype(jnp.int32)
        picks[which] = (slot_col == at_slot).astype(F32).astype(BF16)
    weight0 = columns[:, 2:3]
    weight1 = columns[:, 3:4]

    forward_own(members(0))
    forward_far(members(0))
    forward_own(members(2))
    for load in loads[7:10]:
        load.wait()
    arrived(0)
    experts(0)
    send_near(0)
    forward_far(members(2))
    arrived(2)
    forward_own(members(3)[:half_chunk])
    experts(2)
    send_near(2)
    send_far(0)

    inc[...] = jnp.zeros_like(inc)
    for k in range(n_ep - 1, 0, -1):

        @pl.when(e >= k)
        def _():
            for copy in state_copies(k, e):
                copy.wait_recv()
            inc[...] = inc[...] * fade_recv[k, 0:1, :] + st_recv[k].astype(F32)

    def final_pass(b, before_log):
        at = pl.ds(pl.multiple_of(b * BLOCK, BLOCK), BLOCK)
        cum = cum_s[at, :]
        ahead = (q_s[at, :].astype(F32) * jnp.exp(cum)).astype(BF16)
        behind = (k_s[at, :].astype(F32) * jnp.exp(-cum)).astype(BF16)
        entry = (state_s[b] + inc[...] * jnp.exp(before_log)).astype(BF16)
        for h in range(heads):
            cols = slice(h * VALUE_DIM, (h + 1) * VALUE_DIM)
            own = jnp.where(head_of == h, ahead, jnp.zeros_like(ahead))
            scores = jnp.where(causal, dot_t(own, behind, ((1,), (1,))), 0.0)
            attended = dot(scores.astype(BF16), v_s[at, cols]) + dot_t(own, entry, ((1,), (1,)))
            gate = g_s[at, cols]
            gated[at, cols] = (
                attended
                * rms_scale(attended)
                * head_gain[:, cols]
                * (gate * jax.nn.sigmoid(gate))
            ).astype(BF16)
        return before_log + cum[BLOCK - 1 : BLOCK, :]

    before_log = lax.fori_loop(0, blocks // 2, final_pass, jnp.zeros((1, keys), F32))
    send_far(2)
    send_back(0)
    lax.fori_loop(blocks // 2, blocks, final_pass, before_log)
    forward_own(members(3)[half_chunk:])
    forward_far(members(3))
    loads[10].wait()
    mix_rows = n_first // n_tp

    def mix(i, carry):
        at = pl.ds(pl.multiple_of(i * mix_rows, mix_rows), mix_rows)
        mixp[i] = dot(gated[at, :], wm[...]).astype(BF16)
        return carry

    lax.fori_loop(0, n_tp, mix, 0)
    mix1 = [
        remote(
            mixp.at[2 * h + near_lo], mrecv1.at[h], m1_ss.at[h], m1_rs.at[h], (e, near)
        )
        for h in range(2)
    ]
    for copy in mix1:
        copy.start()
    send_back(2)
    arrived(3)
    experts(3)
    send_near(3)
    forward_own(members(1))
    forward_far(members(1))
    send_far(3)
    for copy in mix1:
        copy.wait_recv()
    msend[...] = (
        mixp[2 * hi_other + lo].astype(F32) + mrecv1[hi_other].astype(F32)
    ).astype(BF16)
    mix2 = remote(msend, mrecv2, m2_ss.at[0], m2_rs.at[0], (e, far))
    mix2.start()
    arrived(1)
    experts(1)
    send_near(1)
    send_back(3)
    send_far(1)
    mix2.wait_recv()
    out_first[...] = (
        mixp[t].astype(F32) + mrecv1[hi].astype(F32) + mrecv2[...].astype(F32)
    ).astype(BF16)

    send_back(1)

    for j in range(1, n_ep):
        ret[j].wait_recv()
    out_second[...] = (
        dot(picks[0], received[...]) * weight0 + dot(picks[1], received[...]) * weight1
    ).astype(BF16)

    for j in range(n_ep):
        if j > 0:
            disp[j].wait_send()
            ret[j].wait_send()
            cf0[j].wait_send()
            cf1[j].wait_send()
            if j < doubled:
                dup[j].wait_send()
            else:
                xf[j].wait_send()
    for c in range(CHUNKS):
        for copy in r1[c]:
            copy.wait_send()
        r2[c].wait_send()
    for copy in mix1:
        copy.wait_send()
    mix2.wait_send()
    for k in range(1, n_ep):

        @pl.when(e + k < n_ep)
        def _():
            for copy in state_copies(k, e + k):
                copy.wait_send()


def body(
    tokens_first,
    norm_gain_first,
    w_query,
    w_key,
    w_value,
    w_outgate,
    w_decay,
    decay_bias,
    head_gain,
    w_mix_out,
    tokens_second,
    norm_gain_second,
    routes,
    route_logits,
    expert_gate,
    expert_up,
    expert_down,
):
    n_ep = lax.axis_size("ep")
    n_tp = lax.axis_size("tp")
    n_first, model = tokens_first.shape
    n_rows = tokens_second.shape[0]
    room = 2 * routes.shape[1] * n_rows // (n_ep * expert_gate.shape[0])
    n_slots = n_ep * room
    width = model // n_tp
    keys = w_query.shape[1]
    values = w_value.shape[1]
    hidden = expert_gate.shape[2]
    blocks = n_first // BLOCK
    mix_rows = n_first // n_tp
    chunk_rows = n_slots // CHUNKS
    vmem = pltpu.VMEM
    dma = pltpu.SemaphoreType.DMA

    def like(x):
        return vmem(x.shape, x.dtype)

    whole = pl.BlockSpec(memory_space=pltpu.VMEM)
    away = pl.BlockSpec(memory_space=pl.ANY)
    scratch = [
        like(tokens_first),
        like(w_query),
        like(w_key),
        like(w_value),
        like(w_outgate),
        like(w_decay),
        like(w_mix_out),
        like(tokens_second),
        like(expert_gate),
        like(expert_up),
        like(expert_down),
        vmem((n_first, model), BF16),
        vmem((n_first, keys), BF16),
        vmem((n_first, keys), BF16),
        vmem((n_first, values), BF16),
        vmem((n_first, values), F32),
        vmem((n_first, keys), F32),
        vmem((blocks, VALUE_DIM, keys), F32),
        vmem((VALUE_DIM, keys), BF16),
        vmem((8, keys), F32),
        vmem((n_ep, VALUE_DIM, keys), BF16),
        vmem((n_ep, 8, keys), F32),
        vmem((VALUE_DIM, keys), F32),
        vmem((n_first, values), BF16),
        vmem((n_tp, mix_rows, model), BF16),
        vmem((2, mix_rows, model), BF16),
        vmem((mix_rows, model), BF16),
        vmem((mix_rows, model), BF16),
        vmem((2, n_slots, width), BF16),
        vmem((n_tp, n_slots, width), BF16),
        vmem((chunk_rows, hidden), BF16),
        vmem((n_tp, n_slots, width), BF16),
        vmem((2, n_slots, width), BF16),
        vmem((n_slots, width), BF16),
        vmem((n_slots, width), BF16),
        vmem((n_slots, width), BF16),
        vmem((n_slots, width), BF16),
        vmem((2, n_rows, n_slots), BF16),
        dma((11,)),
        dma((n_ep,)),
        dma((n_ep,)),
        dma((n_ep,)),
        dma((n_ep,)),
        dma((n_ep,)),
        dma((n_ep,)),
        dma((n_ep, 2)),
        dma((n_ep, 2)),
        dma((n_ep,)),
        dma((n_ep,)),
        dma((n_ep,)),
        dma((n_ep,)),
        dma((2,)),
        dma((2,)),
        dma((1,)),
        dma((1,)),
        dma((CHUNKS, 2)),
        dma((CHUNKS, 2)),
        dma((CHUNKS,)),
        dma((CHUNKS,)),
        dma((n_ep,)),
        dma((n_ep,)),
    ]
    return pl.pallas_call(
        functools.partial(kernel, n_ep, n_tp),
        out_shape=(
            jax.ShapeDtypeStruct((mix_rows, model), BF16),
            jax.ShapeDtypeStruct((n_rows, width), BF16),
        ),
        in_specs=[away, whole, away, away, away, away, away, whole, whole, away]
        + [away, whole, whole, whole, away, away, away],
        out_specs=(whole, whole),
        scratch_shapes=scratch,
        compiler_params=pltpu.CompilerParams(
            collective_id=0, has_side_effects=True, vmem_limit_bytes=60 * 1024 * 1024
        ),
    )(
        tokens_first,
        norm_gain_first[None, :],
        w_query,
        w_key,
        w_value,
        w_outgate,
        w_decay,
        decay_bias,
        head_gain[None, :],
        w_mix_out,
        tokens_second,
        norm_gain_second[None, :],
        routes.T,
        route_logits.T,
        expert_gate,
        expert_up,
        expert_down,
    )


def solution(mesh):
    in_specs = (
        P("ep", None),
        P(),
        P(None, "tp"),
        P(None, "tp"),
        P(None, "tp"),
        P(None, "tp"),
        P(None, "tp"),
        P("ep", "tp"),
        P("tp"),
        P("tp", None),
        P("ep", None),
        P(),
        P("ep", None),
        P("ep", None),
        P("ep", None, "tp"),
        P("ep", None, "tp"),
        P("ep", "tp", None),
    )
    out_specs = (P(("ep", "tp"), None), P("ep", "tp"))
    return jax.shard_map(body, mesh=mesh, in_specs=in_specs, out_specs=out_specs, check_vma=False)
```

```python
import functools

import jax
import jax.numpy as jnp
from jax import lax
from jax.experimental import pallas as pl
from jax.experimental.pallas import tpu as pltpu
from jax.sharding import PartitionSpec as P

KEY_DIM = 64
VALUE_DIM = 128
BLOCK = 64
EPS = 1e-06
TEMPER = 16.0
CHUNKS = 4
LANES = 128

MESH = pl.DeviceIdType.MESH
F32 = jnp.float32
BF16 = jnp.bfloat16


def flip(index, mask):
    bit = 1
    while bit <= mask:
        if mask & bit:
            index = index + bit - 2 * bit * ((index // bit) % 2)
        bit *= 2
    return index


def dot(a, b):
    return jnp.dot(a, b, preferred_element_type=F32)


def dot_t(a, b, dims):
    return lax.dot_general(a, b, (dims, ((), ())), preferred_element_type=F32)


def rms_scale(wide):
    return lax.rsqrt(jnp.mean(wide * wide, axis=-1, keepdims=True) + EPS)


def kernel(
    n_ep,
    n_tp,
    tokens_first,
    gain_first,
    w_query,
    w_key,
    w_value,
    w_outgate,
    w_decay,
    decay_bias,
    head_gain,
    w_mix_out,
    tokens_second,
    gain_second,
    routes_t,
    logits_t,
    e_gate,
    e_up,
    e_down,
    out_first,
    out_second,
    tf,
    wq,
    wk,
    wv,
    wg,
    wd,
    wm,
    ts,
    eg,
    eu,
    ed,
    normed,
    q_s,
    k_s,
    v_s,
    g_s,
    cum_s,
    state_s,
    st_send,
    fade_send,
    st_recv,
    fade_recv,
    inc,
    gated,
    mixp,
    mrecv1,
    msend,
    mrecv2,
    slots,
    rows,
    hid,
    part,
    recv1,
    send2,
    recv2,
    result,
    received,
    picks,
    load_sem,
    disp_ss,
    disp_rs,
    dup_ss,
    dup_rs,
    xf_ss,
    xf_rs,
    cf_ss,
    cf_rs,
    st_ss,
    st_rs,
    fd_ss,
    fd_rs,
    m1_ss,
    m1_rs,
    m2_ss,
    m2_rs,
    r1_ss,
    r1_rs,
    r2_ss,
    r2_rs,
    ret_ss,
    ret_rs,
):
    e = lax.axis_index("ep")
    t = lax.axis_index("tp")
    lo = t % 2
    hi = t // 2
    near = flip(t, 1)
    far = flip(t, 2)
    cross = flip(t, 3)
    hi_other = 1 - hi

    loads = [
        pltpu.make_async_copy(src, dst, load_sem.at[i])
        for i, (src, dst) in enumerate(
            [
                (tokens_second, ts),
                (tokens_first, tf),
                (w_query, wq),
                (w_key, wk),
                (w_decay, wd),
                (w_value, wv),
                (w_outgate, wg),
                (e_gate, eg),
                (e_up, eu),
                (e_down, ed),
                (w_mix_out, wm),
            ]
        )
    ]
    for load in loads:
        load.start()

    barrier = pltpu.get_barrier_semaphore()
    for j in range(1, n_ep):
        pl.semaphore_signal(barrier, inc=1, device_id=(flip(e, j), t), device_id_type=MESH)
    for peer in (near, far):
        pl.semaphore_signal(barrier, inc=1, device_id=(e, peer), device_id_type=MESH)

    n_rows = ts.shape[0]
    _, n_slots, width = slots.shape
    room = n_slots // n_ep
    expert_col = lax.broadcasted_iota(jnp.int32, (LANES, n_rows), 0)
    rt = routes_t[...]
    m0 = (expert_col == rt[0:1, :]).astype(F32)
    m1 = (expert_col == rt[1:2, :]).astype(F32)
    r_i = lax.broadcasted_iota(jnp.int32, (n_rows, n_rows), 0)
    c_i = lax.broadcasted_iota(jnp.int32, (n_rows, n_rows), 1)
    before = dot((m0 + m1).astype(BF16), (r_i < c_i).astype(BF16))
    t0 = rt[0:1, :] * room + jnp.sum(m0 * before, axis=0, keepdims=True).astype(jnp.int32)
    t1 = rt[1:2, :] * room + jnp.sum(m1 * before, axis=0, keepdims=True).astype(jnp.int32)
    loads[0].wait()
    scale2 = rms_scale(ts[...].astype(F32))

    def features(block):
        cols = pl.ds(pl.multiple_of(block * width, width), width)
        return (ts[:, cols].astype(F32) * scale2 * gain_second[:, cols]).astype(BF16)

    def chosen(start, count):
        slot_id = lax.broadcasted_iota(jnp.int32, (count, n_rows), 0) + start
        return ((slot_id == t0) | (slot_id == t1)).astype(F32).astype(BF16)

    pieces = (features(t), features(far))

    def build(i, carry):
        start = pl.multiple_of(i * 256, 256)
        pick = chosen(start, 256)
        for which in range(2):
            slots[which, pl.ds(start, 256), :] = dot(pick, pieces[which]).astype(BF16)
        return carry

    lax.fori_loop(0, n_slots // 256, build, 0)

    def place(s):
        return pl.ds(pl.multiple_of(s * room, room), room)

    pl.semaphore_wait(barrier, n_ep + 1)

    def remote(src, dst, ss, rs, dev):
        return pltpu.make_async_remote_copy(
            src_ref=src, dst_ref=dst, send_sem=ss, recv_sem=rs, device_id=dev, device_id_type=MESH
        )

    per_chunk = n_ep // CHUNKS

    def members(c):
        return list(range(c * per_chunk, (c + 1) * per_chunk))

    doubled = 2 * per_chunk
    disp, dup = [None], [None]
    for j in range(1, n_ep):
        s = flip(e, j)
        disp.append(
            remote(
                slots.at[0, place(s), :],
                rows.at[t, place(e), :],
                disp_ss.at[j],
                disp_rs.at[j],
                (s, t),
            )
        )
        if j < doubled:
            dup.append(
                remote(
                    slots.at[1, place(s), :],
                    rows.at[far, place(e), :],
                    dup_ss.at[j],
                    dup_rs.at[j],
                    (s, t),
                )
            )

    def dispatch(j):
        disp[j].start()
        if j < doubled:
            dup[j].start()

    half_chunk = per_chunk // 2
    early = members(0)[1:] + members(2) + members(3)[:half_chunk]
    late = members(3)[half_chunk:] + members(1)
    for j in early:
        dispatch(j)
    own_pick = chosen(e * room, room)
    rows[t, place(e), :] = slots[0, place(e), :]
    rows[far, place(e), :] = slots[1, place(e), :]
    rows[near, place(e), :] = dot(own_pick, features(near)).astype(BF16)
    rows[cross, place(e), :] = dot(own_pick, features(cross)).astype(BF16)

    xf, cf0, cf1 = [], [], []
    for j in range(n_ep):
        p = place(flip(e, j))
        xf.append(
            None
            if j < doubled
            else remote(rows.at[t, p, :], rows.at[t, p, :], xf_ss.at[j], xf_rs.at[j], (e, far))
        )
        cf0.append(
            None
            if j == 0
            else remote(
                rows.at[t, p, :], rows.at[t, p, :], cf_ss.at[j, 0], cf_rs.at[j, 0], (e, near)
            )
        )
        cf1.append(
            None
            if j == 0
            else remote(
                rows.at[far, p, :], rows.at[far, p, :], cf_ss.at[j, 1], cf_rs.at[j, 1], (e, near)
            )
        )

    def forward_own(js):
        for j in js:
            if j > 0:
                disp[j].wait_recv()
                if j >= doubled:
                    xf[j].start()
                cf0[j].start()

    def forward_far(js):
        for j in js:
            if j > 0:
                if j < doubled:
                    dup[j].wait_recv()
                else:
                    xf[j].wait_recv()
                cf1[j].start()

    def arrived(c):
        for j in members(c):
            if j > 0:
                cf0[j].wait_recv()
                cf1[j].wait_recv()

    loads[1].wait()
    n_first = tf.shape[0]
    blocks = n_first // BLOCK

    def norm_rows(i, carry):
        at = pl.ds(pl.multiple_of(i * BLOCK, BLOCK), BLOCK)
        wide = tf[at, :].astype(F32)
        normed[at, :] = (wide * rms_scale(wide) * gain_first[...]).astype(BF16)
        return carry

    lax.fori_loop(0, blocks, norm_rows, 0)
    loads[2].wait()
    q_s[...] = (dot(normed[...], wq[...]) * KEY_DIM ** (-0.5)).astype(BF16)
    loads[3].wait()
    k_s[...] = dot(normed[...], wk[...]).astype(BF16)
    loads[4].wait()
    cum_s[...] = dot(normed[...], wd[...])
    loads[5].wait()
    v_s[...] = dot(normed[...], wv[...]).astype(BF16)
    loads[6].wait()
    g_s[...] = dot(normed[...], wg[...])
    forward_own(members(0))
    forward_far(members(0))

    keys = k_s.shape[1]
    heads = keys // KEY_DIM
    tri_r = lax.broadcasted_iota(jnp.int32, (BLOCK, BLOCK), 0)
    tri_c = lax.broadcasted_iota(jnp.int32, (BLOCK, BLOCK), 1)
    causal = tri_r >= tri_c
    tri = causal.astype(F32)
    head_of = lax.broadcasted_iota(jnp.int32, (1, keys), 1) // KEY_DIM
    inc[...] = jnp.zeros_like(inc)

    def local_pass(b, total):
        at = pl.ds(pl.multiple_of(b * BLOCK, BLOCK), BLOCK)
        pre = cum_s[at, :] + decay_bias[pl.ds(b, 1), :]
        log_decay = (jnp.minimum(pre, 0.0) - jnp.log1p(jnp.exp(-jnp.abs(pre)))) / TEMPER
        cum = jnp.dot(tri, log_decay, precision=lax.Precision.HIGHEST, preferred_element_type=F32)
        cum_s[at, :] = cum
        last = cum[BLOCK - 1 : BLOCK, :]
        fading = (k_s[at, :].astype(F32) * jnp.exp(last - cum)).astype(BF16)
        full = dot_t(v_s[at, :], fading, ((0,), (0,)))
        add = full[0:VALUE_DIM]
        for h in range(1, heads):
            add = jnp.where(head_of == h, full[h * VALUE_DIM : (h + 1) * VALUE_DIM], add)
        state_s[b] = inc[...]
        inc[...] = inc[...] * jnp.exp(last) + add
        return total + last

    total = lax.fori_loop(0, blocks, local_pass, jnp.zeros((1, keys), F32))
    st_send[...] = inc[...].astype(BF16)
    fade_send[...] = jnp.broadcast_to(jnp.exp(total), fade_send.shape)

    def state_copies(k, dst):
        return (
            remote(st_send, st_recv.at[k], st_ss.at[k], st_rs.at[k], (dst, t)),
            remote(fade_send, fade_recv.at[k], fd_ss.at[k], fd_rs.at[k], (dst, t)),
        )

    for k in range(1, n_ep):

        @pl.when(e + k < n_ep)
        def _():
            for copy in state_copies(k, e + k):
                copy.start()

    for j in late:
        dispatch(j)

    chunk_rows = n_slots // CHUNKS
    hidden_width = hid.shape[1]
    tile = 256

    def chunk_at(c):
        m = flip(e // per_chunk, c)
        return pl.ds(pl.multiple_of(m * chunk_rows, chunk_rows), chunk_rows)

    def experts(c):
        at = chunk_at(c)

        def up(i, carry):
            cols = pl.ds(pl.multiple_of(i * tile, tile), tile)
            gate = jnp.zeros((chunk_rows, tile), F32)
            upper = jnp.zeros((chunk_rows, tile), F32)
            for b in range(n_tp):
                x = rows[b, at, :]
                gate = gate + dot(x, eg[0, b * width : (b + 1) * width, cols])
                upper = upper + dot(x, eu[0, b * width : (b + 1) * width, cols])
            hid[:, cols] = (gate * jax.nn.sigmoid(gate) * upper).astype(BF16)
            return carry

        lax.fori_loop(0, hidden_width // tile, up, 0)

        def down(b, carry):
            cols = pl.ds(pl.multiple_of(b * width, width), width)
            part[b, at, :] = dot(hid[...], ed[0, :, cols]).astype(BF16)
            return carry

        lax.fori_loop(0, n_tp, down, 0)

    near_lo = 1 - lo
    r1, r2, ret = [], [], []
    for c in range(CHUNKS):
        at = chunk_at(c)
        r1.append(
            [
                remote(
                    part.at[2 * h + near_lo, at, :],
                    recv1.at[h, at, :],
                    r1_ss.at[c, h],
                    r1_rs.at[c, h],
                    (e, near),
                )
                for h in range(2)
            ]
        )
        r2.append(remote(send2.at[at, :], recv2.at[at, :], r2_ss.at[c], r2_rs.at[c], (e, far)))
    for j in range(n_ep):
        s = flip(e, j)
        ret.append(
            remote(
                result.at[place(s), :], received.at[place(e), :], ret_ss.at[j], ret_rs.at[j], (s, t)
            )
        )

    def send_near(c):
        for copy in r1[c]:
            copy.start()

    def send_far(c):
        at = chunk_at(c)
        for copy in r1[c]:
            copy.wait_recv()
        send2[at, :] = (
            part[2 * hi_other + lo, at, :].astype(F32) + recv1[hi_other, at, :].astype(F32)
        ).astype(BF16)
        r2[c].start()

    def send_back(c):
        at = chunk_at(c)
        r2[c].wait_recv()
        result[at, :] = (
            part[t, at, :].astype(F32)
            + recv1[hi, at, :].astype(F32)
            + recv2[at, :].astype(F32)
        ).astype(BF16)
        for j in range(c * per_chunk, (c + 1) * per_chunk):
            if j > 0:
                ret[j].start()
        if c == 0:
            received[place(e), :] = result[place(e), :]

    share0 = jax.nn.sigmoid(logits_t[0:1, :] - logits_t[1:2, :])
    share1 = jax.nn.sigmoid(logits_t[1:2, :] - logits_t[0:1, :])
    stacked = jnp.concatenate(
        [
            t0.astype(F32),
            t1.astype(F32),
            share0,
            share1,
            jnp.zeros((LANES - 4, n_rows), F32),
        ],
        axis=0,
    )
    columns = jnp.transpose(stacked)
    slot_col = lax.broadcasted_iota(jnp.int32, (n_rows, n_slots), 1)
    for which in range(2):
        at_slot = columns[:, which : which + 1].astype(jnp.int32)
        picks[which] = (slot_col == at_slot).astype(F32).astype(BF16)
    weight0 = columns[:, 2:3]
    weight1 = columns[:, 3:4]

    forward_own(members(2))
    for load in loads[7:10]:
        load.wait()
    arrived(0)
    experts(0)
    send_near(0)
    send_far(0)
    forward_far(members(2))
    arrived(2)
    experts(2)
    send_near(2)
    forward_own(members(3)[:half_chunk])
    send_far(2)
    send_back(0)

    inc[...] = jnp.zeros_like(inc)
    for k in range(n_ep - 1, 0, -1):

        @pl.when(e >= k)
        def _():
            for copy in state_copies(k, e):
                copy.wait_recv()
            inc[...] = inc[...] * fade_recv[k, 0:1, :] + st_recv[k].astype(F32)

    def final_pass(b, before_log):
        at = pl.ds(pl.multiple_of(b * BLOCK, BLOCK), BLOCK)
        cum = cum_s[at, :]
        ahead = (q_s[at, :].astype(F32) * jnp.exp(cum)).astype(BF16)
        behind = (k_s[at, :].astype(F32) * jnp.exp(-cum)).astype(BF16)
        entry = (state_s[b] + inc[...] * jnp.exp(before_log)).astype(BF16)
        for h in range(heads):
            cols = slice(h * VALUE_DIM, (h + 1) * VALUE_DIM)
            own = jnp.where(head_of == h, ahead, jnp.zeros_like(ahead))
            scores = jnp.where(causal, dot_t(own, behind, ((1,), (1,))), 0.0)
            attended = dot(scores.astype(BF16), v_s[at, cols]) + dot_t(own, entry, ((1,), (1,)))
            gate = g_s[at, cols]
            gated[at, cols] = (
                attended
                * rms_scale(attended)
                * head_gain[:, cols]
                * (gate * jax.nn.sigmoid(gate))
            ).astype(BF16)
        return before_log + cum[BLOCK - 1 : BLOCK, :]

    lax.fori_loop(0, blocks, final_pass, jnp.zeros((1, keys), F32))
    loads[10].wait()
    mix_rows = n_first // n_tp

    def mix(i, carry):
        at = pl.ds(pl.multiple_of(i * mix_rows, mix_rows), mix_rows)
        mixp[i] = dot(gated[at, :], wm[...]).astype(BF16)
        return carry

    lax.fori_loop(0, n_tp, mix, 0)
    mix1 = [
        remote(
            mixp.at[2 * h + near_lo], mrecv1.at[h], m1_ss.at[h], m1_rs.at[h], (e, near)
        )
        for h in range(2)
    ]
    for copy in mix1:
        copy.start()
    forward_own(members(3)[half_chunk:])
    forward_own(members(1))
    forward_far(members(1))
    arrived(1)
    for copy in mix1:
        copy.wait_recv()
    msend[...] = (
        mixp[2 * hi_other + lo].astype(F32) + mrecv1[hi_other].astype(F32)
    ).astype(BF16)
    half_mix = mix_rows // 2
    mix2 = []
    for h in range(2):
        at = pl.ds(h * half_mix, half_mix)
        mix2.append(
            remote(msend.at[at, :], mrecv2.at[at, :], m2_ss.at[h], m2_rs.at[h], (e, far))
        )
    mix2[0].start()
    experts(1)
    send_near(1)
    send_back(2)
    send_far(1)
    forward_far(members(3))
    arrived(3)
    experts(3)
    send_near(3)
    send_back(1)
    send_far(3)
    send_back(3)
    mix2[1].start()
    for copy in mix2:
        copy.wait_recv()
    out_first[...] = (
        mixp[t].astype(F32) + mrecv1[hi].astype(F32) + mrecv2[...].astype(F32)
    ).astype(BF16)

    for j in range(1, n_ep):
        ret[j].wait_recv()
    out_second[...] = (
        dot(picks[0], received[...]) * weight0 + dot(picks[1], received[...]) * weight1
    ).astype(BF16)

    for j in range(n_ep):
        if j > 0:
            disp[j].wait_send()
            ret[j].wait_send()
            cf0[j].wait_send()
            cf1[j].wait_send()
            if j < doubled:
                dup[j].wait_send()
            else:
                xf[j].wait_send()
    for c in range(CHUNKS):
        for copy in r1[c]:
            copy.wait_send()
        r2[c].wait_send()
    for copy in mix1:
        copy.wait_send()
    for copy in mix2:
        copy.wait_send()
    for k in range(1, n_ep):

        @pl.when(e + k < n_ep)
        def _():
            for copy in state_copies(k, e + k):
                copy.wait_send()


def body(
    tokens_first,
    norm_gain_first,
    w_query,
    w_key,
    w_value,
    w_outgate,
    w_decay,
    decay_bias,
    head_gain,
    w_mix_out,
    tokens_second,
    norm_gain_second,
    routes,
    route_logits,
    expert_gate,
    expert_up,
    expert_down,
):
    n_ep = lax.axis_size("ep")
    n_tp = lax.axis_size("tp")
    n_first, model = tokens_first.shape
    n_rows = tokens_second.shape[0]
    room = 2 * routes.shape[1] * n_rows // (n_ep * expert_gate.shape[0])
    n_slots = n_ep * room
    width = model // n_tp
    keys = w_query.shape[1]
    values = w_value.shape[1]
    hidden = expert_gate.shape[2]
    blocks = n_first // BLOCK
    mix_rows = n_first // n_tp
    chunk_rows = n_slots // CHUNKS
    vmem = pltpu.VMEM
    dma = pltpu.SemaphoreType.DMA

    def like(x):
        return vmem(x.shape, x.dtype)

    whole = pl.BlockSpec(memory_space=pltpu.VMEM)
    away = pl.BlockSpec(memory_space=pl.ANY)
    scratch = [
        like(tokens_first),
        like(w_query),
        like(w_key),
        like(w_value),
        like(w_outgate),
        like(w_decay),
        like(w_mix_out),
        like(tokens_second),
        like(expert_gate),
        like(expert_up),
        like(expert_down),
        vmem((n_first, model), BF16),
        vmem((n_first, keys), BF16),
        vmem((n_first, keys), BF16),
        vmem((n_first, values), BF16),
        vmem((n_first, values), F32),
        vmem((n_first, keys), F32),
        vmem((blocks, VALUE_DIM, keys), F32),
        vmem((VALUE_DIM, keys), BF16),
        vmem((8, keys), F32),
        vmem((n_ep, VALUE_DIM, keys), BF16),
        vmem((n_ep, 8, keys), F32),
        vmem((VALUE_DIM, keys), F32),
        vmem((n_first, values), BF16),
        vmem((n_tp, mix_rows, model), BF16),
        vmem((2, mix_rows, model), BF16),
        vmem((mix_rows, model), BF16),
        vmem((mix_rows, model), BF16),
        vmem((2, n_slots, width), BF16),
        vmem((n_tp, n_slots, width), BF16),
        vmem((chunk_rows, hidden), BF16),
        vmem((n_tp, n_slots, width), BF16),
        vmem((2, n_slots, width), BF16),
        vmem((n_slots, width), BF16),
        vmem((n_slots, width), BF16),
        vmem((n_slots, width), BF16),
        vmem((n_slots, width), BF16),
        vmem((2, n_rows, n_slots), BF16),
        dma((11,)),
        dma((n_ep,)),
        dma((n_ep,)),
        dma((n_ep,)),
        dma((n_ep,)),
        dma((n_ep,)),
        dma((n_ep,)),
        dma((n_ep, 2)),
        dma((n_ep, 2)),
        dma((n_ep,)),
        dma((n_ep,)),
        dma((n_ep,)),
        dma((n_ep,)),
        dma((2,)),
        dma((2,)),
        dma((2,)),
        dma((2,)),
        dma((CHUNKS, 2)),
        dma((CHUNKS, 2)),
        dma((CHUNKS,)),
        dma((CHUNKS,)),
        dma((n_ep,)),
        dma((n_ep,)),
    ]
    return pl.pallas_call(
        functools.partial(kernel, n_ep, n_tp),
        out_shape=(
            jax.ShapeDtypeStruct((mix_rows, model), BF16),
            jax.ShapeDtypeStruct((n_rows, width), BF16),
        ),
        in_specs=[away, whole, away, away, away, away, away, whole, whole, away]
        + [away, whole, whole, whole, away, away, away],
        out_specs=(whole, whole),
        scratch_shapes=scratch,
        compiler_params=pltpu.CompilerParams(
            collective_id=0, has_side_effects=True, vmem_limit_bytes=60 * 1024 * 1024
        ),
    )(
        tokens_first,
        norm_gain_first[None, :],
        w_query,
        w_key,
        w_value,
        w_outgate,
        w_decay,
        decay_bias,
        head_gain[None, :],
        w_mix_out,
        tokens_second,
        norm_gain_second[None, :],
        routes.T,
        route_logits.T,
        expert_gate,
        expert_up,
        expert_down,
    )


def solution(mesh):
    in_specs = (
        P("ep", None),
        P(),
        P(None, "tp"),
        P(None, "tp"),
        P(None, "tp"),
        P(None, "tp"),
        P(None, "tp"),
        P("ep", "tp"),
        P("tp"),
        P("tp", None),
        P("ep", None),
        P(),
        P("ep", None),
        P("ep", None),
        P("ep", None, "tp"),
        P("ep", None, "tp"),
        P("ep", "tp", None),
    )
    out_specs = (P(("ep", "tp"), None), P("ep", "tp"))
    return jax.shard_map(body, mesh=mesh, in_specs=in_specs, out_specs=out_specs, check_vma=False)
```
